32 devices in a mesh: sp: 8 (over z, y), tp: 4 (over x, core).
Axes of the slice: x: 2, y: 2, z: 4, core: 2. Of those that a mesh axis runs over, the one named last changes fastest.
Arguments:
- queries: bfloat16 [2048, 2048], P('sp', 'tp'), may hold values from -6 to 6
- key_value: bfloat16 [2048, 4, 128], P('sp', 'tp'), may hold values from -12 to 12
- break_bias: bfloat16 [2048, 32], P('sp', 'tp'), may hold values from -13 to 0
- stream: bfloat16 [2048, 2048], P(('sp', 'tp')), may hold values from -6 to 6
- out_proj: bfloat16 [2048, 2048], replicated, may hold values from -0.125 to 0.125
- ffn_gain: float32 [2048], replicated, may hold values from 0.1 to 1.9
- routes: int32 [2048, 4], P(('sp', 'tp')), may hold values from 0 to 31, all different within a row; in each aligned block of 64 rows (0 to 63, 64 to 127, ...) at most 16 rows name the same one
- route_score: float32 [2048, 4], P(('sp', 'tp')), may hold values from 0.05 to 1
- expert_gate: bfloat16 [32, 2048, 512], P(('sp', 'tp')), may hold values from -0.125 to 0.125
- expert_up: bfloat16 [32, 2048, 512], P(('sp', 'tp')), may hold values from -0.125 to 0.125
- expert_down: bfloat16 [32, 512, 2048], P(('sp', 'tp')), may hold values from -0.25 to 0.25
- shared_gate: bfloat16 [2048, 512], replicated, may hold values from -0.125 to 0.125
- shared_up: bfloat16 [2048, 512], replicated, may hold values from -0.125 to 0.125
- shared_down: bfloat16 [512, 2048], replicated, may hold values from -0.25 to 0.25
Outputs:
- layer_out: bfloat16 [2048, 2048], P(('sp', 'tp'))
The draws below stay inside these ranges and needn't reach their ends.
Inputs may be any that keep to these rules, and one draw needn't show every extreme that they name: `routes`: each row names 4 different experts. In each aligned block of 64 rows (the rows of one device) no expert is named by more than 16 rows, a bound that some block reaches.
All inputs are finite; a program needn't handle non-finite values.
Results may differ from the reference program's by a relative error of at most 0.015.
Values may be sent and summed in bfloat16 or wider, within the bound.
A program may use at most 128 MiB of HBM per device.

```python
import math
import jax
import jax.numpy as jnp
import numpy as np
from jax import lax

D = 2048
QUERY_HEADS = 32
KV_HEADS = 4
HD = 64
EFF = 512
SFF = 512
TOPK = 4
KEY_BLOCK = 1024
TOK_DEV = 256
SEQUENCE_TOKENS = 2048
ROWS_DEV = 64
EXPERTS = 32
CAP = 16


def draw_key_value(key, part):
    key_one, key_two, key_three = jax.random.split(jax.random.fold_in(key, 11), 3)
    block_total = SEQUENCE_TOKENS // TOK_DEV
    key_part = jax.random.normal(key_one, (SEQUENCE_TOKENS, KV_HEADS, HD), jnp.float32)
    noise_level = 1.5 * jax.random.normal(key_two, (block_total, 1, KV_HEADS, HD), jnp.float32)
    noise = jax.random.normal(key_three, (block_total, TOK_DEV, KV_HEADS, HD), jnp.float32)
    value_part = (noise_level + noise).reshape(SEQUENCE_TOKENS, KV_HEADS, HD)
    joined = jnp.concatenate([key_part, value_part], axis=2)
    return jnp.clip(joined, -12.0, 12.0).astype(jnp.bfloat16)


def draw_break_bias(key, part):
    key_vectors = jax.random.split(jax.random.fold_in(key, 23), 5)
    block_total = SEQUENCE_TOKENS // TOK_DEV
    fast_share = 0.5
    fast = jax.random.uniform(key_vectors[0], (QUERY_HEADS,), jnp.float32) < fast_share
    slow_level = -jnp.log(1.65 * SEQUENCE_TOKENS)
    noise_level = jnp.where(fast, jnp.log(1.0 / 40.0), slow_level)
    block_offset = jax.random.uniform(key_vectors[1], (block_total, 1, QUERY_HEADS), jnp.float32, -0.7, 0.7)
    block_offset = jnp.broadcast_to(block_offset, (block_total, TOK_DEV, QUERY_HEADS)).reshape(SEQUENCE_TOKENS, QUERY_HEADS)
    coarse_noise = jax.random.uniform(key_vectors[2], (SEQUENCE_TOKENS, QUERY_HEADS), jnp.float32, -0.5, 0.5)
    sudden_spike = jax.random.uniform(key_vectors[3], (SEQUENCE_TOKENS, QUERY_HEADS), jnp.float32) < 2.0 / SEQUENCE_TOKENS
    spike_value = jax.random.uniform(key_vectors[4], (SEQUENCE_TOKENS, QUERY_HEADS), jnp.float32, -1.4, 0.0)
    offset_rows = jnp.where(sudden_spike, spike_value, noise_level[None, :] + block_offset + coarse_noise)
    return jnp.clip(offset_rows, -13.0, 0.0).astype(jnp.bfloat16)


def block_levels(key, dims, shards, low, high):
    def one(dim, blocks):
        heights = jax.random.uniform(jax.random.fold_in(jax.random.fold_in(key, 6), dim), (blocks,), jnp.float32, low / len(shards), high / len(shards))
        return jnp.repeat(jnp.exp(heights), dims[dim] // blocks).reshape((-1,) + (1,) * (len(dims) - dim - 1))

    gain = one(*shards[0])
    for cut in shards[1:]:
        gain = gain * one(*cut)
    return gain


def assign_block(key, own, number, rows, number_of, top, bound, slope):
    order = jax.random.permutation(key, number_of)
    crowded, common = portions_of(number_of, rows * top, bound, slope, True), portions_of(number_of, rows * top, bound, slope, False)
    places = jnp.arange(number_of)

    def named(lengths, turn):
        used = int((lengths > 0).sum())
        fixed = max(1, used // 4)
        moved = fixed + (places - fixed + turn * (used - fixed)) % max(1, number_of - fixed)
        return jnp.zeros((number_of,), jnp.int32).at[order[jnp.where(places < fixed, places, moved)]].set(jnp.asarray(lengths, jnp.int32))

    lengths = jnp.where(number % 4 == 0, named(crowded, number // 4), named(common, number - number // 4 - 1))
    mixed = jax.random.permutation(jax.random.fold_in(own, 3), number_of)
    giver, sink = mixed[0:number_of // 2 * 2:2], mixed[1:number_of // 2 * 2:2]
    room = jnp.minimum(lengths[giver] - 1, bound - lengths[sink]) // 2
    room = jnp.where((giver == order[0]) | (sink == order[0]) | (lengths[sink] == 0), 0, jnp.maximum(room, 0))
    moved = jax.random.randint(jax.random.fold_in(own, 4), (number_of // 2,), 0, 1 << 20) % (room + 1)
    lengths = lengths.at[giver].add(-moved).at[sink].add(moved)
    items = jnp.searchsorted(jnp.cumsum(lengths), jnp.arange(rows * top), side="right").astype(jnp.int32)
    grid = items.reshape(top, rows).T
    grid = grid[jax.random.permutation(jax.random.fold_in(own, 1), rows)]
    turn = jax.random.randint(jax.random.fold_in(own, 2), (rows, 1), 0, top)
    return jnp.take_along_axis(grid, (jnp.arange(top)[None, :] + turn) % top, axis=1)


def portions_of(count, total, limit, skew, full):
    portions = [(1 << 20) // math.isqrt(standing ** skew) + 1 for standing in range(1, count + 1)]
    largest = limit if full else min(limit, max(-(-total // count), total * portions[0] // sum(portions)))
    least = 1 if total - largest >= count - 1 else 0
    holding, surplus = [largest] + [least] * (count - 1), total - largest - least * (count - 1)
    while surplus > 0:
        candidates = [i for i in range(1, count) if holding[i] < largest] or [i for i in range(1, count) if holding[i] < limit]
        whole, remaining = sum([portions[i] for i in candidates]), surplus
        for i in candidates:
            addition = min(limit - holding[i], max(1, remaining * portions[i] // whole), surplus)
            holding[i] = holding[i] + addition
            surplus = surplus - addition
    return np.array(holding)


def bell_draw(own_key, shape, spread, limit, pieces=(), held_as=jnp.bfloat16):
    gain = block_levels(own_key, shape, pieces, -0.22, 0.18) if pieces else 1.0
    result = jax.random.normal(own_key, shape, jnp.float32) * spread * gain
    return jnp.minimum(jnp.maximum(result, -limit), limit).astype(held_as)


def setup_inputs(seed: int = 0) -> dict:
    keys = jax.random.split(jax.random.key(seed), 15)
    queries = bell_draw(keys[0], (SEQUENCE_TOKENS, QUERY_HEADS * HD), 1.0, 6.0, ((0, 8), (1, 4)))
    key_value = draw_key_value(jax.random.fold_in(keys[14], 71), 0)
    break_bias = draw_break_bias(jax.random.fold_in(keys[14], 71), 0)
    stream = bell_draw(keys[3], (SEQUENCE_TOKENS, D), 1.0, 6.0, ((0, 32),))
    out_proj = bell_draw(keys[4], (QUERY_HEADS * HD, D), (QUERY_HEADS * HD) ** -0.5, 0.125)
    ffn_gain = jnp.clip(1.0 + 0.18 * jax.random.normal(keys[5], (D,), jnp.float32), 0.1, 1.9)
    routes_keys = jax.random.split(jax.random.fold_in(keys[6], 1), SEQUENCE_TOKENS // ROWS_DEV)
    routes_turns = jax.random.permutation(jax.random.fold_in(keys[6], 3), SEQUENCE_TOKENS // ROWS_DEV)
    routes = jax.vmap(lambda own, number: assign_block(jax.random.fold_in(keys[6], 2), own, number, ROWS_DEV, EXPERTS, TOPK, CAP, 2))(routes_keys, routes_turns).reshape((SEQUENCE_TOKENS, TOPK))
    route_score = jnp.clip(jnp.exp(math.log(1.0) - 2.9957323 * jax.random.uniform(keys[7], (SEQUENCE_TOKENS, TOPK), jnp.float32) ** block_levels(keys[7], (SEQUENCE_TOKENS, TOPK), ((0, 32),), -0.2, 0.2)), 0.05, 1.0)
    expert_gate = bell_draw(keys[8], (EXPERTS, D, EFF), D ** -0.5, 0.125, ((0, 32),))
    expert_up = bell_draw(keys[9], (EXPERTS, D, EFF), D ** -0.5, 0.125, ((0, 32),))
    expert_down = bell_draw(keys[10], (EXPERTS, EFF, D), EFF ** -0.5, 0.25, ((0, 32),))
    shared_gate = bell_draw(keys[11], (D, SFF), D ** -0.5, 0.125)
    shared_up = bell_draw(keys[12], (D, SFF), D ** -0.5, 0.125)
    shared_down = bell_draw(keys[13], (SFF, D), SFF ** -0.5, 0.25)
    return {"queries": queries, "key_value": key_value, "break_bias": break_bias, "stream": stream, "out_proj": out_proj, "ffn_gain": ffn_gain, "routes": routes, "route_score": route_score, "expert_gate": expert_gate, "expert_up": expert_up, "expert_down": expert_down, "shared_gate": shared_gate, "shared_up": shared_up, "shared_down": shared_down}


def pad_front(values, count):
    filler = jnp.zeros((count,) + values.shape[1:], values.dtype)
    return jnp.concatenate([filler, values], axis=0)

def stick_sweep(query_block, key_value, break_bias, query_start, key_block):
    query_rows, kv_heads, group_size, head_size = query_block.shape
    scale = head_size ** (-0.5)
    query_pos = query_start + jnp.arange(query_rows, dtype=jnp.int32)
    query_end = query_start + query_rows
    block_count = (query_end + key_block - 1) // key_block
    query_wide = query_block.astype(jnp.float32)

    def one_block(block_index, carry):
        output, carried = carry
        key_start = (query_end - (block_index + 1) * key_block).astype(jnp.int32)
        rows_here = lax.dynamic_slice_in_dim(key_value, key_start + key_block, key_block, 0)
        shift_here = lax.dynamic_slice_in_dim(break_bias, key_start + key_block, key_block, 0).astype(jnp.float32)
        key_part = rows_here[..., :head_size].astype(jnp.float32)
        value_part = rows_here[..., head_size:].astype(jnp.float32)
        logits = jnp.einsum('qhgd,khd->hgqk', query_wide, key_part) * scale
        logits = logits + jnp.transpose(shift_here, (1, 2, 0))[:, :, None, :]
        key_pos = key_start + jnp.arange(key_block, dtype=jnp.int32)
        valid = (key_pos[None, :] < query_pos[:, None]) & (key_pos[None, :] >= 0)
        log_stay = jnp.where(valid, jax.nn.log_sigmoid(-logits), 0.0)
        beyond = lax.cumsum(log_stay, axis=3, reverse=True) - log_stay + carried[..., None]
        weight = jnp.where(valid, jnp.exp(jax.nn.log_sigmoid(logits) + beyond), 0.0)
        weight = lax.optimization_barrier(weight.astype(jnp.bfloat16)).astype(jnp.float32)
        output = output + jnp.einsum('hgqk,khd->qhgd', weight, value_part)
        return (output, carried + lax.optimization_barrier(jnp.sum(log_stay, axis=3)))
    start_state = (jnp.zeros((query_rows, kv_heads, group_size, head_size), jnp.float32), jnp.zeros((kv_heads, group_size, query_rows), jnp.float32))
    output, _ = lax.fori_loop(0, block_count, one_block, start_state)
    return output.astype(jnp.bfloat16).reshape(query_rows, kv_heads * group_size * head_size)

def rms_scale(resid, ffn_gain):
    wide = resid.astype(jnp.float32)
    factor = lax.rsqrt(lax.optimization_barrier(jnp.mean(wide * wide, axis=-1, keepdims=True)) + 1e-06)
    return (wide * factor * ffn_gain).astype(jnp.bfloat16)

def reference(queries, key_value, break_bias, stream, out_proj, ffn_gain, routes, route_score, expert_gate, expert_up, expert_down, shared_gate, shared_up, shared_down):
    group_size = QUERY_HEADS // KV_HEADS
    query_grid = queries.reshape(SEQUENCE_TOKENS // TOK_DEV, TOK_DEV, KV_HEADS, group_size, HD)
    padded_kv = pad_front(key_value, KEY_BLOCK)
    padded_bias = pad_front(break_bias.reshape(SEQUENCE_TOKENS, KV_HEADS, group_size), KEY_BLOCK)
    starts = jnp.arange(SEQUENCE_TOKENS // TOK_DEV, dtype=jnp.int32) * TOK_DEV

    def sweep_block(packed):
        return stick_sweep(packed[0], padded_kv, padded_bias, packed[1], KEY_BLOCK)
    attended = lax.map(sweep_block, (query_grid, starts)).reshape(SEQUENCE_TOKENS, QUERY_HEADS * HD)
    mixed = jnp.dot(attended, out_proj, preferred_element_type=jnp.float32)
    resid = (stream.astype(jnp.float32) + mixed).astype(jnp.bfloat16)
    normed = rms_scale(resid, ffn_gain)
    gates = 2.5 * route_score / lax.optimization_barrier(jnp.sum(route_score, axis=1, keepdims=True))
    flat_expert = routes.reshape(-1).astype(jnp.int32)
    flat_row = jnp.repeat(jnp.arange(SEQUENCE_TOKENS, dtype=jnp.int32), TOPK)
    onehot = (flat_expert[:, None] == jnp.arange(EXPERTS, dtype=jnp.int32)[None, :]).astype(jnp.int32)
    rank = lax.optimization_barrier(jnp.sum((jnp.cumsum(onehot, axis=0) - onehot) * onehot, axis=1)).astype(jnp.int32)
    slot_count = SEQUENCE_TOKENS // ROWS_DEV * CAP
    row_table = jnp.full((EXPERTS, slot_count), SEQUENCE_TOKENS, jnp.int32).at[flat_expert, rank].set(flat_row)
    gate_table = jnp.zeros((EXPERTS, slot_count), jnp.float32).at[flat_expert, rank].set(gates.reshape(-1))
    normed_pad = jnp.concatenate([normed, jnp.zeros((1, D), normed.dtype)], axis=0)

    def expert_step(total, packed):
        row_ids, gate_ids, w_gate, w_up, w_down = packed
        chosen = normed_pad[row_ids]
        gate_part = jnp.dot(chosen, w_gate, preferred_element_type=jnp.float32)
        up_part = jnp.dot(chosen, w_up, preferred_element_type=jnp.float32)
        inner = (jax.nn.silu(gate_part) * up_part).astype(jnp.bfloat16)
        done = jnp.dot(inner, w_down, preferred_element_type=jnp.float32).astype(jnp.bfloat16)
        return (total.at[row_ids].add(gate_ids[:, None] * done.astype(jnp.float32)), None)
    routed, _ = lax.scan(expert_step, jnp.zeros((SEQUENCE_TOKENS + 1, D), jnp.float32), (row_table, gate_table, expert_gate, expert_up, expert_down))
    shared_inner = (jax.nn.silu(jnp.dot(normed, shared_gate, preferred_element_type=jnp.float32)) * jnp.dot(normed, shared_up, preferred_element_type=jnp.float32)).astype(jnp.bfloat16)
    shared_out = jnp.dot(shared_inner, shared_down, preferred_element_type=jnp.float32)
    return (resid.astype(jnp.float32) + shared_out + routed[:SEQUENCE_TOKENS]).astype(jnp.bfloat16)
```

```python
import functools
import math

import jax
import jax.numpy as jnp
from jax import lax
from jax.experimental import pallas as pl
from jax.experimental.pallas import tpu as pltpu
from jax.sharding import PartitionSpec as P

MESH = pl.DeviceIdType.MESH
LOG2E = math.log2(math.e)
HEADS_AT_ONCE = 4


def gather_kernel(seq, half, packed_ref, query_ref, route_ref, every_ref, far_ref, plans_ref,
                  send, recv, q_send, q_recv, r_send, r_recv):
    me = lax.axis_index("sp")
    partner = me + 1 - 2 * (me % 2)
    mirror = seq - 1 - me
    barrier = pltpu.get_barrier_semaphore()
    for step in range(1, seq):
        pl.semaphore_signal(
            barrier, inc=1, device_id={"sp": (me + step) % seq}, device_id_type=MESH
        )
    pl.semaphore_wait(barrier, seq - 1)

    def push(source, block, target, slot):
        return pltpu.make_async_remote_copy(
            src_ref=source,
            dst_ref=every_ref.at[block],
            send_sem=send.at[slot],
            recv_sem=recv.at[block],
            device_id={"sp": target},
            device_id_type=MESH,
        )

    steps = seq // 2
    first = [push(packed_ref, me, partner, 0)]
    for step in range(1, steps):
        first.append(push(packed_ref, me, (me + 2 * step) % seq, step))
    for copy in first:
        copy.start()
    send_start = jnp.where(me < seq // 2, half, 0)
    moving = pltpu.make_async_remote_copy(
        src_ref=query_ref.at[pl.ds(pl.multiple_of(send_start, half), half)],
        dst_ref=far_ref,
        send_sem=q_send,
        recv_sem=q_recv,
        device_id={"sp": mirror},
        device_id_type=MESH,
    )
    moving.start()

    def tell(step):
        return pltpu.make_async_remote_copy(
            src_ref=route_ref,
            dst_ref=plans_ref.at[me],
            send_sem=r_send.at[step],
            recv_sem=r_recv.at[me],
            device_id={"sp": (me + step) % seq},
            device_id_type=MESH,
        )

    for step in range(1, seq):
        tell(step).start()
    plans_ref[me] = route_ref[...]
    every_ref[me] = packed_ref[...]
    relayed = []
    for step in range(1, steps):
        block = (me + seq - 2 * step) % seq
        copy = push(every_ref.at[block], block, partner, steps + step)
        push(packed_ref, block, partner, 0).wait_recv()
        copy.start()
        relayed.append(copy)
    for step in range(steps):
        block = (partner + seq - 2 * step) % seq
        push(packed_ref, block, partner, 0).wait_recv()
    moving.wait_recv()
    for step in range(1, seq):
        block = (me + step) % seq
        pltpu.make_async_remote_copy(
            src_ref=route_ref,
            dst_ref=plans_ref.at[block],
            send_sem=r_send.at[step],
            recv_sem=r_recv.at[block],
            device_id={"sp": block},
            device_id_type=MESH,
        ).wait_recv()
    for copy in first + relayed:
        copy.wait_send()
    for step in range(1, seq):
        tell(step).wait_send()
    moving.wait_send()


def gather_keys(packed, queries, route, seq):
    half = queries.shape[0] // 2
    vmem = pl.BlockSpec(memory_space=pltpu.VMEM)
    return pl.pallas_call(
        functools.partial(gather_kernel, seq, half),
        out_shape=(
            jax.ShapeDtypeStruct((seq,) + packed.shape, packed.dtype),
            jax.ShapeDtypeStruct((half, queries.shape[1]), queries.dtype),
            jax.ShapeDtypeStruct((seq,) + route.shape, route.dtype),
        ),
        in_specs=[vmem, vmem, vmem],
        out_specs=(vmem, vmem, vmem),
        scratch_shapes=[
            pltpu.SemaphoreType.DMA((seq,)),
            pltpu.SemaphoreType.DMA((seq,)),
            pltpu.SemaphoreType.DMA,
            pltpu.SemaphoreType.DMA,
            pltpu.SemaphoreType.DMA((seq,)),
            pltpu.SemaphoreType.DMA((seq,)),
        ],
        compiler_params=pltpu.CompilerParams(collective_id=0, has_side_effects=True),
        name="gather_keys",
    )(packed, queries, route)


def stick_kernel(seq, heads, head_size, bias_rows, query_ref, far_ref, every_ref, out_ref,
                 lhs, after, carried, total):
    me = lax.axis_index("sp")
    half = far_ref.shape[0]
    keys = every_ref.shape[2]
    depth = head_size + bias_rows
    scale = head_size ** (-0.5) * LOG2E
    keep_start = jnp.where(me < seq // 2, 0, half)
    row_id = lax.broadcasted_iota(jnp.int32, (keys, keys), 0)
    col_id = lax.broadcasted_iota(jnp.int32, (keys, keys), 1)
    after[...] = jnp.where(row_id > col_id, 1.0, 0.0).astype(jnp.bfloat16)
    group = HEADS_AT_ONCE
    rows = group * half
    mark = lax.broadcasted_iota(jnp.int32, (half, bias_rows), 1)
    for part in range(2):
        for head in range(heads):
            columns = slice(head * head_size, (head + 1) * head_size)
            if part == 0:
                mine = query_ref[pl.ds(pl.multiple_of(keep_start, half), half), columns]
            else:
                mine = far_ref[:, columns]
            at = pl.ds(head * half, half)
            lhs[at, 0:head_size] = mine
            lhs[at, head_size:depth] = jnp.where(mark == head, 1.0, 0.0).astype(jnp.bfloat16)
        owner = me if part == 0 else seq - 1 - me

        def sweep(block, diagonal):
            for turn in range(heads // group):
                at = pl.ds(turn * rows, rows)
                logits = (
                    jnp.dot(
                        lhs[at, :],
                        every_ref[block, 0:depth, :],
                        preferred_element_type=jnp.float32,
                    )
                    * scale
                )
                soft = jnp.maximum(logits, 0.0) + jnp.log2(1.0 + jnp.exp2(-jnp.abs(logits)))
                take = logits - soft
                if diagonal:
                    row = lax.broadcasted_iota(jnp.int32, (rows, keys), 0) % half + keep_start
                    valid = lax.broadcasted_iota(jnp.int32, (rows, keys), 1) < row
                    soft = jnp.where(valid, soft, 0.0)
                beyond = jnp.dot(
                    soft.astype(jnp.bfloat16), after[...], preferred_element_type=jnp.float32
                )
                if diagonal:
                    weight = jnp.where(valid, jnp.exp2(take - beyond), 0.0)
                else:
                    weight = jnp.exp2(take - (beyond + carried[at, :]))
                product = lax.dot_general(
                    weight.astype(jnp.bfloat16),
                    every_ref[block, depth : depth + head_size, :],
                    (((1,), (1,)), ((), ())),
                    preferred_element_type=jnp.float32,
                )
                here = beyond[:, 0:1] + soft[:, 0:1]
                if diagonal:
                    total[at, :] = product
                    carried[at, :] = here
                else:
                    total[at, :] += product
                    carried[at, :] += here

        sweep(owner, True)

        @pl.loop(0, owner)
        def _(step):
            sweep(owner - 1 - step, False)

        for head in range(heads):
            out_ref[part * half : (part + 1) * half, head * head_size : (head + 1) * head_size] = (
                total[head * half : (head + 1) * half, :].astype(jnp.bfloat16)
            )


def stick_attention(queries, far, every, heads, head_size, bias_rows):
    vmem = pl.BlockSpec(memory_space=pltpu.VMEM)
    seq, _, keys = every.shape
    half = far.shape[0]
    elements = 9 * heads * half * keys
    return pl.pallas_call(
        functools.partial(stick_kernel, seq, heads, head_size, bias_rows),
        out_shape=jax.ShapeDtypeStruct(queries.shape, queries.dtype),
        in_specs=[vmem] * 3,
        out_specs=vmem,
        scratch_shapes=[
            pltpu.VMEM((heads * half, head_size + bias_rows), jnp.bfloat16),
            pltpu.VMEM((keys, keys), jnp.bfloat16),
            pltpu.VMEM((heads * half, 1), jnp.float32),
            pltpu.VMEM((heads * half, head_size), jnp.float32),
        ],
        cost_estimate=pl.CostEstimate(
            flops=2 * elements * (keys + 2 * head_size),
            bytes_accessed=2 * every.size,
            transcendentals=3 * elements,
        ),
        name="stick_attention",
    )(queries, far, every)


def owners_kernel(seq, ranks, part_ref, out_ref, send, recv, local):
    me, rank = lax.axis_index("sp"), lax.axis_index("tp")
    mirror = seq - 1 - me
    chunk = out_ref.shape[0]
    width = part_ref.shape[1]
    barrier = pltpu.get_barrier_semaphore()
    for step in range(1, ranks):
        pl.semaphore_signal(
            barrier,
            inc=1,
            device_id={"sp": me, "tp": (rank + step) % ranks},
            device_id_type=MESH,
        )
    for step in range(ranks):
        pl.semaphore_signal(
            barrier, inc=1, device_id={"sp": mirror, "tp": step}, device_id_type=MESH
        )
    pl.semaphore_wait(barrier, 2 * ranks - 1)
    half = ranks // 2
    first = jnp.where(me < seq // 2, 0, half)
    place = pl.ds(pl.multiple_of(rank * width, width), width)

    def push(index, owner, target):
        return pltpu.make_async_remote_copy(
            src_ref=part_ref.at[pl.ds(index * chunk, chunk)],
            dst_ref=out_ref.at[:, place],
            send_sem=send.at[index],
            recv_sem=recv.at[rank],
            device_id={"sp": owner, "tp": target},
            device_id_type=MESH,
        )

    def stays(index):
        return pltpu.make_async_copy(
            part_ref.at[pl.ds(index * chunk, chunk)], out_ref.at[:, place], local
        )

    for index in range(half, ranks):
        push(index, mirror, first + index - half).start()
    for index in range(half):
        target = first + index

        @pl.when(target != rank)
        def _():
            push(index, me, target).start()

        @pl.when(target == rank)
        def _():
            stays(index).start()

    kept = (rank // half) * half == first

    for source in range(ranks):

        @pl.when(jnp.logical_not(jnp.logical_and(kept, rank == source)))
        def _():
            pltpu.make_async_remote_copy(
                src_ref=part_ref.at[pl.ds(0, chunk)],
                dst_ref=out_ref.at[:, source * width : (source + 1) * width],
                send_sem=send.at[0],
                recv_sem=recv.at[source],
                device_id={"sp": mirror, "tp": source},
                device_id_type=MESH,
            ).wait_recv()

    for index in range(half, ranks):
        push(index, mirror, first + index - half).wait_send()
    for index in range(half):
        target = first + index

        @pl.when(target != rank)
        def _():
            push(index, me, target).wait_send()

        @pl.when(target == rank)
        def _():
            stays(index).wait()


def to_owners(part, seq, ranks):
    vmem = pl.BlockSpec(memory_space=pltpu.VMEM)
    rows, width = part.shape
    return pl.pallas_call(
        functools.partial(owners_kernel, seq, ranks),
        out_shape=jax.ShapeDtypeStruct((rows // ranks, width * ranks), part.dtype),
        in_specs=[vmem],
        out_specs=vmem,
        scratch_shapes=[
            pltpu.SemaphoreType.DMA((ranks,)),
            pltpu.SemaphoreType.DMA((ranks,)),
            pltpu.SemaphoreType.DMA,
        ],
        compiler_params=pltpu.CompilerParams(collective_id=1, has_side_effects=True),
        name="to_owners",
    )(part)


def moe_kernel(seq, ranks, top, cap, resid_ref, gain_ref, plans_ref, gate_hbm, up_hbm, down_hbm,
               s_gate_hbm, s_up_hbm, s_down_hbm, out_ref, w_gate, w_up, w_down, v_gate, v_up,
               v_down, rows, stage, arrived, done, back, part, land, base, inner, loads, z_send,
               z_recv, d_send, d_recv, b_send, b_recv, l_send, l_recv):
    me, rank = lax.axis_index("sp"), lax.axis_index("tp")
    line = seq // 2
    z, y = me // 2, me % 2
    plane = 2 * ranks
    mine = y * ranks + rank
    count, width = resid_ref.shape
    slots = plane * cap
    piece = width // l_send.shape[1]
    barrier = pltpu.get_barrier_semaphore()
    for step in range(1, plane):
        other = (mine + step) % plane
        pl.semaphore_signal(
            barrier,
            inc=1,
            device_id={"sp": 2 * z + other // ranks, "tp": other % ranks},
            device_id_type=MESH,
        )

    @pl.when(z > 0)
    def _():
        pl.semaphore_signal(barrier, inc=1, device_id={"sp": me - 2}, device_id_type=MESH)

    @pl.when(z < line - 1)
    def _():
        pl.semaphore_signal(barrier, inc=1, device_id={"sp": me + 2}, device_id_type=MESH)

    pairs = [
        (s_gate_hbm, v_gate),
        (s_up_hbm, v_up),
        (s_down_hbm, v_down),
        (gate_hbm, w_gate),
        (up_hbm, w_up),
        (down_hbm, w_down),
    ]
    fetches = [
        pltpu.make_async_copy(source, target, loads.at[index])
        for index, (source, target) in enumerate(pairs)
    ]
    for fetch in fetches:
        fetch.start()

    wide = resid_ref[...].astype(jnp.float32)
    factor = lax.rsqrt(jnp.mean(wide * wide, axis=-1, keepdims=True) + 1e-06)
    rows[z] = (wide * factor * gain_ref[...]).astype(jnp.bfloat16)
    pl.semaphore_wait(
        barrier,
        plane - 1 + jnp.where(z > 0, 1, 0) + jnp.where(z < line - 1, 1, 0),
    )

    def block_at(k):
        low, high = z, line - 1 - z
        both = jnp.minimum(low, high)
        near = jnp.where(k % 2 == 1, z + (k + 1) // 2, z - (k + 1) // 2)
        far = jnp.where(low > high, z - (k - both), z + (k - both))
        return jnp.where(k <= 2 * both, near, far)

    def shift(block, way):
        return pltpu.make_async_remote_copy(
            src_ref=rows.at[block],
            dst_ref=rows.at[block],
            send_sem=z_send.at[block, (way + 1) // 2],
            recv_sem=z_recv.at[block],
            device_id={"sp": me + 2 * way},
            device_id_type=MESH,
        )

    def inside(block, way):
        low = z - 1 >= 0 if way < 0 else z + 1 < line
        return jnp.logical_and(low, block >= z if way < 0 else block <= z)

    def forward(block, act):
        for way in (-1, 1):

            @pl.when(inside(block, way))
            def _(way=way):
                act(shift(block, way))

    def hand(source, target, block, step, sends, recvs):
        other = (mine + step) % plane
        return pltpu.make_async_remote_copy(
            src_ref=source.at[block, other],
            dst_ref=target.at[block, mine],
            send_sem=sends.at[block, step],
            recv_sem=recvs.at[block],
            device_id={"sp": 2 * z + other // ranks, "tp": other % ranks},
            device_id_type=MESH,
        )

    def gathered(target, block, recvs):
        return pltpu.make_async_remote_copy(
            src_ref=target.at[block, pl.ds(0, plane - 1)],
            dst_ref=target.at[block, pl.ds(0, plane - 1)],
            send_sem=z_send.at[0, 0],
            recv_sem=recvs.at[block],
            device_id={"tp": (rank + 1) % ranks},
            device_id_type=MESH,
        )

    def slot_grid(block):
        plan = plans_ref[2 * block + y]
        spots = lax.broadcasted_iota(jnp.int32, (slots, count), 0) + z * slots
        return plan, spots

    def send_rows(block):
        plan, spots = slot_grid(block)
        hit = None
        for k in range(top):
            same = plan[k : k + 1, :].astype(jnp.int32) == spots
            hit = same if hit is None else jnp.logical_or(hit, same)
        pick = jnp.where(hit, 1.0, 0.0).astype(jnp.bfloat16)
        for start in range(0, width, 512):
            columns = slice(start, start + 512)
            packed = jnp.dot(
                pick, rows[block, :, columns], preferred_element_type=jnp.float32
            ).astype(jnp.bfloat16)
            for other in range(plane):
                stage[block, other, :, columns] = packed[other * cap : (other + 1) * cap]
        for step in range(1, plane):
            hand(stage, arrived, block, step, d_send, d_recv).start()
        arrived[block, mine] = stage[block, mine]

    def join(source, block, columns=slice(None)):
        return jnp.concatenate(
            [source[block, other, :, columns] for other in range(plane)], axis=0
        )

    def expert(block):
        gathered(arrived, block, d_recv).wait_recv()
        taken = join(arrived, block)
        hidden = w_gate.shape[1]
        for start in range(0, hidden, 256):
            columns = slice(start, start + 256)
            gate = jnp.dot(taken, w_gate[:, columns], preferred_element_type=jnp.float32)
            up = jnp.dot(taken, w_up[:, columns], preferred_element_type=jnp.float32)
            inner[0:slots, columns] = (jax.nn.silu(gate) * up).astype(jnp.bfloat16)
        for start in range(0, width, 512):
            columns = slice(start, start + 512)
            result = jnp.dot(
                inner[0:slots, :], w_down[:, columns], preferred_element_type=jnp.float32
            ).astype(jnp.bfloat16)
            for other in range(plane):
                done[block, other, :, columns] = result[other * cap : (other + 1) * cap]

    def give_back(block):
        for step in range(1, plane):
            hand(done, back, block, step, b_send, b_recv).start()
        back[block, mine] = done[block, mine]

    def weights_of(block):
        plan, spots = slot_grid(block)
        total = jnp.zeros((slots, count), jnp.float32)
        for k in range(top):
            same = plan[k : k + 1, :].astype(jnp.int32) == spots
            total = total + jnp.where(same, plan[top + k : top + k + 1, :], 0.0)
        turned = total.T
        coarse = turned.astype(jnp.bfloat16)
        return coarse, (turned - coarse.astype(jnp.float32)).astype(jnp.bfloat16)

    def summed(coarse, fine, block, columns):
        taken = join(back, block, columns)
        return jnp.dot(coarse, taken, preferred_element_type=jnp.float32) + jnp.dot(
            fine, taken, preferred_element_type=jnp.float32
        )

    def pass_on(block, way, index):
        target = z + way
        slot = jnp.where(jnp.logical_and(way < 0, block == target), line, block)
        at = pl.ds(index * piece, piece)
        return pltpu.make_async_remote_copy(
            src_ref=part.at[block, :, at],
            dst_ref=land.at[slot, :, at],
            send_sem=l_send.at[block, index],
            recv_sem=l_recv.at[slot, index],
            device_id={"sp": me + 2 * way},
            device_id_type=MESH,
        )

    def landed(slot, index):
        at = pl.ds(index * piece, piece)
        return pltpu.make_async_remote_copy(
            src_ref=land.at[slot, :, at],
            dst_ref=land.at[slot, :, at],
            send_sem=z_send.at[0, 0],
            recv_sem=l_recv.at[slot, index],
            device_id={"tp": (rank + 1) % ranks},
            device_id_type=MESH,
        )

    pieces = [(index, slice(index * piece, (index + 1) * piece)) for index in range(width // piece)]

    def collect(block):
        way = jnp.where(block > z, 1, -1)
        behind = jnp.where(block > z, z > 0, z < line - 1)
        coarse, fine = weights_of(block)
        gathered(back, block, b_recv).wait_recv()
        for index, columns in pieces:
            here = summed(coarse, fine, block, columns)

            @pl.when(behind)
            def _():
                landed(block, index).wait_recv()
                part[block, :, columns] = (
                    here + land[block, :, columns].astype(jnp.float32)
                ).astype(jnp.bfloat16)

            @pl.when(jnp.logical_not(behind))
            def _():
                part[block, :, columns] = here.astype(jnp.bfloat16)

            pass_on(block, way, index).start()

    forward(z, lambda copy: copy.start())
    send_rows(z)

    for fetch in fetches[:3]:
        fetch.wait()
    normed = rows[z]
    shared = v_gate.shape[1]
    for start in range(0, shared, 256):
        columns = slice(start, start + 256)
        gate = jnp.dot(normed, v_gate[:, columns], preferred_element_type=jnp.float32)
        up = jnp.dot(normed, v_up[:, columns], preferred_element_type=jnp.float32)
        inner[0:count, columns] = (jax.nn.silu(gate) * up).astype(jnp.bfloat16)
    for start in range(0, width, 512):
        columns = slice(start, start + 512)
        base[:, columns] = resid_ref[:, columns].astype(jnp.float32) + jnp.dot(
            inner[0:count, :], v_down[:, columns], preferred_element_type=jnp.float32
        )
    for fetch in fetches[3:]:
        fetch.wait()

    @pl.loop(1, line)
    def _(k):
        block = block_at(k)
        pltpu.make_async_remote_copy(
            src_ref=rows.at[block],
            dst_ref=rows.at[block],
            send_sem=z_send.at[0, 0],
            recv_sem=z_recv.at[block],
            device_id={"tp": (rank + 1) % ranks},
            device_id_type=MESH,
        ).wait_recv()
        forward(block, lambda copy: copy.start())
        send_rows(block)
        expert(block_at(k - 1))

    expert(block_at(line - 1))

    @pl.loop(0, line)
    def _(k):
        give_back(block_at(line - 1 - k))

    @pl.loop(0, line - 1)
    def _(k):
        collect(block_at(line - 1 - k))

    coarse, fine = weights_of(z)
    gathered(back, z, b_recv).wait_recv()
    for index, columns in pieces:
        base[:, columns] += summed(coarse, fine, z, columns)

    for index, columns in pieces:
        for present, slot in ((z > 0, z), (z < line - 1, line)):

            @pl.when(present)
            def _(slot=slot):
                landed(slot, index).wait_recv()
                base[:, columns] += land[slot, :, columns].astype(jnp.float32)

        out_ref[:, columns] = base[:, columns].astype(jnp.bfloat16)

    @pl.loop(0, line)
    def _(block):
        forward(block, lambda copy: copy.wait_send())
        for step in range(1, plane):
            hand(stage, arrived, block, step, d_send, d_recv).wait_send()
            hand(done, back, block, step, b_send, b_recv).wait_send()

        @pl.when(block != z)
        def _():
            for index, _ in pieces:
                pass_on(block, jnp.where(block > z, 1, -1), index).wait_send()


def moe(resid, gain, plans, experts, shared, seq, ranks, top):
    vmem = pl.BlockSpec(memory_space=pltpu.VMEM)
    hbm = pl.BlockSpec(memory_space=pl.ANY)
    count, width = resid.shape
    line, plane = seq // 2, 2 * ranks
    cap = 2 * count * top // (seq * ranks)
    pieces = 4
    packed = pltpu.VMEM((line, plane, cap, width), jnp.bfloat16)
    lined = pltpu.VMEM((line, count, width), jnp.bfloat16)
    copies = pltpu.SemaphoreType.DMA
    inner = (max(plane * cap, count), max(experts[0].shape[1], shared[0].shape[1]))
    return pl.pallas_call(
        functools.partial(moe_kernel, seq, ranks, top, cap),
        out_shape=jax.ShapeDtypeStruct(resid.shape, resid.dtype),
        in_specs=[vmem] * 3 + [hbm] * 6,
        out_specs=vmem,
        scratch_shapes=[pltpu.VMEM(w.shape, w.dtype) for w in experts + shared]
        + [lined]
        + [packed] * 4
        + [
            lined,
            pltpu.VMEM((line + 1, count, width), jnp.bfloat16),
            pltpu.VMEM((count, width), jnp.float32),
            pltpu.VMEM(inner, jnp.bfloat16),
            copies((6,)),
            copies((line, 2)),
            copies((line,)),
            copies((line, plane)),
            copies((line,)),
            copies((line, plane)),
            copies((line,)),
            copies((line, pieces)),
            copies((line + 1, pieces)),
        ],
        compiler_params=pltpu.CompilerParams(collective_id=2, has_side_effects=True),
        name="moe",
    )(resid, gain, plans, *experts, *shared)


def body(
    queries,
    key_value,
    break_bias,
    stream,
    out_proj,
    ffn_gain,
    routes,
    route_score,
    expert_gate,
    expert_up,
    expert_down,
    shared_gate,
    shared_up,
    shared_down,
):
    kv_local = key_value.shape[1]
    head_size = key_value.shape[2] // 2
    group_size = break_bias.shape[1] // kv_local
    bias_rows = -(-group_size // 16) * 16
    shift = (break_bias.astype(jnp.float32) * head_size**0.5).astype(jnp.bfloat16)
    joined = key_value[:, 0, :].T
    packed = jnp.concatenate(
        [
            joined[:head_size],
            jnp.pad(shift.T, ((0, bias_rows - group_size), (0, 0))),
            joined[head_size:],
        ],
        axis=0,
    )
    gates = 2.5 * route_score / jnp.sum(route_score, axis=1, keepdims=True)
    row_count, top_count = routes.shape
    seq_count = lax.axis_size("sp")
    rank_count = lax.axis_size("tp")
    expert_count = seq_count * rank_count
    capacity = 2 * row_count * top_count // expert_count
    flat_expert = routes.reshape(-1)
    onehot = (flat_expert[:, None] == jnp.arange(expert_count, dtype=jnp.int32)[None, :]).astype(
        jnp.int32
    )
    rank = jnp.sum((jnp.cumsum(onehot, axis=0) - onehot) * onehot, axis=1)
    slot_ids = (flat_expert * capacity + rank).reshape(row_count, top_count)
    route_plan = jnp.concatenate([slot_ids.astype(jnp.float32).T, gates.T], axis=0)
    every, far, plans = gather_keys(packed, queries, route_plan, seq_count)
    attended = stick_attention(queries, far, every, group_size, head_size, bias_rows)
    token_heads = to_owners(attended, seq_count, rank_count)
    mixed = jnp.dot(token_heads, out_proj, preferred_element_type=jnp.float32)
    resid = (stream.astype(jnp.float32) + mixed).astype(jnp.bfloat16)
    return moe(
        resid,
        ffn_gain[None, :],
        plans,
        (expert_gate[0], expert_up[0], expert_down[0]),
        (shared_gate, shared_up, shared_down),
        seq_count,
        rank_count,
        top_count,
    )


def solution(mesh):
    return jax.shard_map(
        body,
        mesh=mesh,
        in_specs=(
            P("sp", "tp"),
            P("sp", "tp", None),
            P("sp", "tp"),
            P(("sp", "tp"), None),
            P(),
            P(),
            P(("sp", "tp"), None),
            P(("sp", "tp"), None),
            P(("sp", "tp"), None, None),
            P(("sp", "tp"), None, None),
            P(("sp", "tp"), None, None),
            P(),
            P(),
            P(),
        ),
        out_specs=P(("sp", "tp"), None),
        check_vma=False,
    )
```
